32 devices in a mesh: grp: 2 (over x), ra: 4 (over y, core), cb: 4 (over z).
Axes of the slice: x: 2, y: 2, z: 4, core: 2. Of those that a mesh axis runs over, the one named last changes fastest.
Arguments:
- tokens_in: bfloat16 [1024, 2048], P('grp', 'ra'), parts along dimension 0, may hold values from -40 to 40
- first_gain: float32 [2048], P('ra'), may hold values from 0.1 to 1.9
- first_gate: float32 [2048, 5632], P('ra', 'cb'), may hold values from -0.125 to 0.125
- first_gate_scale: float32 [5632], P('cb'), may hold values from 0.1 to 1.9
- first_up: float32 [2048, 5632], P('ra', 'cb'), may hold values from -0.125 to 0.125
- first_up_scale: float32 [5632], P('cb'), may hold values from 0.1 to 1.9
- first_down: float32 [5632, 2048], P('cb', 'ra'), may hold values from -0.078125 to 0.078125
- first_down_scale: float32 [2048], P('ra'), may hold values from 0.1 to 1.9
- second_gain: float32 [2048], P('ra'), may hold values from 0.1 to 1.9
- second_gate: float32 [2048, 5632], P('ra', 'cb'), may hold values from -0.125 to 0.125
- second_gate_scale: float32 [5632], P('cb'), may hold values from 0.1 to 1.9
- second_up: float32 [2048, 5632], P('ra', 'cb'), may hold values from -0.125 to 0.125
- second_up_scale: float32 [5632], P('cb'), may hold values from 0.1 to 1.9
- second_down: float32 [5632, 2048], P('cb', 'ra'), may hold values from -0.078125 to 0.078125
- second_down_scale: float32 [2048], P('ra'), may hold values from 0.1 to 1.9
Outputs:
- tokens_out: bfloat16 [1024, 2048], P('grp', 'ra'), parts along dimension 0
The draws below stay inside these ranges and needn't reach their ends.
There are 2 independent parts, one for each index of `grp`. The reference program is written for one: setup_inputs(seed, part) draws one part's arguments, and reference() takes and returns one part's arrays. A program takes and returns all parts, laid end to end along the dimension named above; an argument that names none is the same for every part. Nothing has to cross between parts.
All inputs are finite; a program needn't handle non-finite values.
Results may differ from the reference program's by a relative error of at most 0.04.
Values may be sent and summed in bfloat16 or wider, within the bound.
A program may use at most 64 MiB of HBM per device.

```python
import math
import jax
import jax.numpy as jnp
from jax import lax

D = 2048
FF = 5632
TOKENS = 512
FF_BLK = 1408
N_CB = 4


def draw_tokens_in(key, part):
    first_key, second_key = jax.random.split(key)
    rows = jnp.exp(jax.random.uniform(first_key, (TOKENS, 1), jnp.float32, math.log(0.3), math.log(3.0)))
    base = jnp.clip(jax.random.normal(second_key, (TOKENS, D), jnp.float32), -4.0, 4.0)
    columns = 1.0 + 2.0 * jnp.arange(D, dtype=jnp.float32)[None, :] / (D - 1)
    return (base * rows * columns).astype(jnp.bfloat16)


def block_levels(stream_key, extent, shards, least, largest):
    def one(axis_at, blocks):
        heights = jax.random.uniform(jax.random.fold_in(jax.random.fold_in(stream_key, 6), axis_at), (blocks,), jnp.float32, least / len(shards), largest / len(shards))
        return jnp.repeat(jnp.exp(heights), extent[axis_at] // blocks).reshape((-1,) + (1,) * (len(extent) - axis_at - 1))

    level = one(*shards[0])
    for cut in shards[1:]:
        level = level * one(*cut)
    return level


def scatter_about(stream_key, extent, spread, reach, pieces=(), kind=jnp.bfloat16):
    drawn = spread * jax.random.normal(stream_key, extent, jnp.float32)
    if pieces:
        drawn = drawn * block_levels(stream_key, extent, pieces, -0.22, 0.18)
    return jnp.clip(drawn, -reach, reach).astype(kind)


def setup_inputs(seed: int = 0, part: int = 0) -> dict:
    seeds = jax.random.split(jax.random.key(seed), 16)
    own_keys = jax.random.split(jax.random.fold_in(seeds[15], part), 16)
    tokens_in = draw_tokens_in(jax.random.fold_in(jax.random.fold_in(seeds[15], part), 71), part)
    first_gain = jnp.clip(1.0 + 0.18 * jax.random.normal(seeds[1], (D,), jnp.float32), 0.1, 1.9)
    first_gate = scatter_about(seeds[2], (D, FF), D ** -0.5, 0.125, ((0, 4), (1, 4)), jnp.float32)
    first_gate_scale = jnp.clip(1.0 + 0.18 * jax.random.normal(seeds[3], (FF,), jnp.float32), 0.1, 1.9)
    first_up = scatter_about(seeds[4], (D, FF), D ** -0.5, 0.125, ((0, 4), (1, 4)), jnp.float32)
    first_up_scale = jnp.clip(1.0 + 0.18 * jax.random.normal(seeds[5], (FF,), jnp.float32), 0.1, 1.9)
    first_down = scatter_about(seeds[6], (FF, D), FF ** -0.5, 0.078125, ((0, 4), (1, 4)), jnp.float32)
    first_down_scale = jnp.clip(1.0 + 0.18 * jax.random.normal(seeds[7], (D,), jnp.float32), 0.1, 1.9)
    second_gain = jnp.clip(1.0 + 0.18 * jax.random.normal(seeds[8], (D,), jnp.float32), 0.1, 1.9)
    second_gate = scatter_about(seeds[9], (D, FF), D ** -0.5, 0.125, ((0, 4), (1, 4)), jnp.float32)
    second_gate_scale = jnp.clip(1.0 + 0.18 * jax.random.normal(seeds[10], (FF,), jnp.float32), 0.1, 1.9)
    second_up = scatter_about(seeds[11], (D, FF), D ** -0.5, 0.125, ((0, 4), (1, 4)), jnp.float32)
    second_up_scale = jnp.clip(1.0 + 0.18 * jax.random.normal(seeds[12], (FF,), jnp.float32), 0.1, 1.9)
    second_down = scatter_about(seeds[13], (FF, D), FF ** -0.5, 0.078125, ((0, 4), (1, 4)), jnp.float32)
    second_down_scale = jnp.clip(1.0 + 0.18 * jax.random.normal(seeds[14], (D,), jnp.float32), 0.1, 1.9)
    return {"tokens_in": tokens_in, "first_gain": first_gain, "first_gate": first_gate, "first_gate_scale": first_gate_scale, "first_up": first_up, "first_up_scale": first_up_scale, "first_down": first_down, "first_down_scale": first_down_scale, "second_gain": second_gain, "second_gate": second_gate, "second_gate_scale": second_gate_scale, "second_up": second_up, "second_up_scale": second_up_scale, "second_down": second_down, "second_down_scale": second_down_scale}


def half_step(acts, gain, gate_w, gate_s, up_w, up_s, down_w, down_s):
    acts_f = acts.astype(jnp.float32)
    mean_sq = lax.optimization_barrier(jnp.sum(acts_f * acts_f, axis=1, keepdims=True)) / D
    factor = lax.rsqrt(mean_sq + 1e-06)
    normed = (acts_f * gain).astype(jnp.bfloat16)
    gate = jnp.dot(normed, gate_w.astype(jnp.bfloat16), preferred_element_type=jnp.float32) * factor * gate_s
    up = jnp.dot(normed, up_w.astype(jnp.bfloat16), preferred_element_type=jnp.float32) * factor * up_s
    hidden = (jax.nn.silu(gate) * up).astype(jnp.bfloat16)
    blocks = hidden.reshape(TOKENS, N_CB, FF_BLK).astype(jnp.float32)
    weights = down_w.astype(jnp.bfloat16).astype(jnp.float32).reshape(N_CB, FF_BLK, D)
    partial_value = jnp.einsum('tcf,cfd->ctd', blocks, weights)
    partial_value = lax.optimization_barrier(partial_value.astype(jnp.bfloat16)).astype(jnp.float32)
    down = lax.optimization_barrier(jnp.sum(partial_value, axis=0)) * down_s
    return (0.5 * acts_f + 0.5 * down).astype(jnp.bfloat16)

def reference(tokens_in, first_gain, first_gate, first_gate_scale, first_up, first_up_scale, first_down, first_down_scale, second_gain, second_gate, second_gate_scale, second_up, second_up_scale, second_down, second_down_scale):
    middle = half_step(tokens_in, first_gain, first_gate, first_gate_scale, first_up, first_up_scale, first_down, first_down_scale)
    return half_step(middle, second_gain, second_gate, second_gate_scale, second_up, second_up_scale, second_down, second_down_scale)
```

```python
import functools

import jax
import jax.numpy as jnp
from jax import lax
from jax.experimental import pallas as pl
from jax.experimental.pallas import tpu as pltpu
from jax.sharding import PartitionSpec as P

MESH = pl.DeviceIdType.MESH
F32 = jnp.float32
BF16 = jnp.bfloat16
LANES = 128
CORES = 2
OFFSETS = (0, 8.06, 18.65, 25.98, 30.61, 35.63, 45.65)
PERIOD = 6.99
LAYER = 55.9


def kernel(cfg, *refs):
    (C, NY, NZ, T, Dk, F, Fp, D) = cfg
    (x_hbm, g1, gs1, us1, ds1, g2, gs2, us2, ds2, wg1, wu1, wd1, wg2, wu2, wd2, out_ref) = refs[:16]
    (x_ref, gain_v, gsc_v, usc_v, dsc_v,
     stage_g, stage_u, stage_d, wcat, wdn, nbuf, own, own2, sA, rA, sB, rB, H, PD, rD, sX, rX, M,
     isem, vsem, wsem, as_, ar_, bs_, br_, cs_, cr_, ps_, pr_, ds_, dr_, xs_, xr_, es_, er_) = refs[16:]
    half = T // CORES
    tr = half // NY
    G = 2 * Fp
    TW = 256 if G % 256 == 0 else LANES
    TD = min(256, Dk)

    ra = lax.axis_index("ra")
    z = lax.axis_index("cb")
    core = lax.rem(ra, CORES)
    y = lax.div(ra, CORES)
    partner = y * CORES + (1 - core)

    def ypeer(d):
        return lax.rem(y + d, NY)

    def zpeer(d):
        return lax.rem(z + d, NZ)

    m1, m2 = NZ // 2 - 1, NZ // 2
    left = z <= m1
    side = jnp.where(left, 0, 1)
    middle = jnp.logical_or(z == m1, z == m2)
    end = jnp.logical_or(z == 0, z == NZ - 1)
    inner = jnp.where(left, z + 1, z - 1)
    not_end, not_middle = jnp.logical_not(end), jnp.logical_not(middle)
    mine_rows = pl.ds(pl.multiple_of(side * half, 16), half)
    other_rows = pl.ds(pl.multiple_of((1 - side) * half, 16), half)

    barrier = pltpu.get_barrier_semaphore()
    pl.semaphore_signal(barrier, inc=1, device_id={"ra": partner}, device_id_type=MESH)
    for d in range(1, NY):
        pl.semaphore_signal(barrier, inc=1, device_id={"ra": ypeer(d) * CORES + core}, device_id_type=MESH)
    for d in range(1, NZ):
        pl.semaphore_signal(barrier, inc=1, device_id={"cb": zpeer(d)}, device_id_type=MESH)

    PARTS = 4
    step = Dk // PARTS
    loads = {}
    inputs = [pltpu.make_async_copy(x_hbm, x_ref, isem)]
    for l, (g, gs, us, ds) in enumerate(((g1, gs1, us1, ds1), (g2, gs2, us2, ds2))):
        for k, (src, dst) in enumerate(((g, gain_v), (gs, gsc_v), (us, usc_v), (ds, dsc_v))):
            inputs.append(pltpu.make_async_copy(src, dst.at[l, pl.ds(0, src.shape[0])], vsem.at[l, k]))
    for l, (a, b, c) in enumerate(((wg1, wu1, wd1), (wg2, wu2, wd2))):
        for k, (src, dst) in enumerate(((a, stage_g), (b, stage_u))):
            for i in range(PARTS):
                r = pl.ds(i * step, step)
                loads[l, k, i] = pltpu.make_async_copy(src.at[r], dst.at[l, r], wsem.at[l, k, i])
        loads[l, 2] = pltpu.make_async_copy(c, stage_d.at[l], wsem.at[l, 2, 0])
    for i in range(PARTS):
        for k in range(2):
            loads[0, k, i].start()
        if i == 0:
            for copy in inputs:
                copy.start()

    def load_rest():
        loads[0, 2].start()
        for k in range(2):
            for i in range(PARTS):
                loads[1, k, i].start()
        loads[1, 2].start()

    def cast_up(l):
        rows = 16
        if F != Fp:
            for k in range(2):
                wcat[l, :, k * Fp + Fp - LANES:(k + 1) * Fp] = jnp.zeros((Dk, LANES), BF16)
        for i in range(PARTS):
            for k, st in ((0, stage_g), (1, stage_u)):
                loads[l, k, i].wait()

                def body(j, _, i=i, k=k, st=st):
                    r = pl.ds(pl.multiple_of(i * step + j * rows, rows), rows)
                    wcat[l, r, k * Fp:k * Fp + F] = st[l, r, :].astype(BF16)
                    return 0

                lax.fori_loop(0, step // rows, body, 0)

    def cast_down(l):
        rows = 32
        loads[l, 2].wait()
        if F != Fp:
            wdn[l, F:, :] = jnp.zeros((Fp - F, Dk), BF16)

        def body(i, _):
            r = pl.ds(pl.multiple_of(i * rows, rows), rows)
            wdn[l, r, :] = stage_d[l, r, :].astype(BF16)
            return 0

        lax.fori_loop(0, F // rows, body, 0)

    flight = {}

    def send(key, src, dst, ssem, rsem, **to):
        copy = pltpu.make_async_remote_copy(
            src_ref=src, dst_ref=dst, send_sem=ssem, recv_sem=rsem, device_id=to, device_id_type=MESH
        )
        copy.start()
        flight[key] = copy

    def ready(src, dst, ssem, rsem, **to):
        return pltpu.make_async_remote_copy(
            src_ref=src, dst_ref=dst, send_sem=ssem, recv_sem=rsem, device_id=to, device_id_type=MESH
        )

    def all_sent(ref, ssem):
        pltpu.make_async_remote_copy(
            src_ref=ref, dst_ref=ref, send_sem=ssem, recv_sem=ar_.at[0, 0], device_id={"ra": partner}, device_id_type=MESH
        ).wait_send()

    def wait_half(l, c, rows, h):
        pltpu.make_async_remote_copy(
            src_ref=M.at[l, c, rows], dst_ref=M.at[l, c, rows], send_sem=es_.at[0], recv_sem=er_.at[l, c, h],
            device_id={"cb": inner}, device_id_type=MESH
        ).wait_recv()

    def split(total):
        hi = total.astype(BF16).astype(F32)
        lane = lax.broadcasted_iota(jnp.int32, (total.shape[0], LANES), 1)
        return jnp.where(lane < LANES // 2, hi, total - hi)

    def acts_rows(l, c, start, n):
        if l == 0:
            return x_ref[pl.ds(pl.multiple_of(c * T + start, 16), n), :]
        return M[0, c, pl.ds(pl.multiple_of(start, 16), n), :]

    def stage_a(l, c):
        slot = c
        if l:
            arrived(0, c)
        squares = []
        gain = gain_v[l, :].reshape(1, Dk)
        for k, h in ((0, 1 - core), (1, core)):
            a = acts_rows(l, c, h * half, half).astype(F32)
            squares.append(jnp.sum(a * a, axis=1, keepdims=True))
            nbuf[k * half:(k + 1) * half, :] = (a * gain).astype(BF16)

        def body(j, _):
            cols = pl.ds(pl.multiple_of(j * TW, TW), TW)
            r = jnp.dot(nbuf[...], wcat[l, :, cols], preferred_element_type=F32)
            sA[l, c, :, cols] = r[:half].astype(BF16)
            own[slot, :, cols] = r[half:]
            return 0

        lax.fori_loop(0, G // TW, body, 0, unroll=True)
        sA[l, c, :, G:] = split(squares[0]).astype(BF16)
        own[slot, :, G:] = split(squares[1])
        send(("a", l, c), sA.at[l, c], rA.at[l, c], as_, ar_.at[l, c], ra=partner)

    def stage_b(l, c):
        slot = c
        flight["a", l, c].wait_recv()

        def reduced(p, store, last):
            r = pl.ds(pl.multiple_of(p * tr, 16), tr)

            def body(j, _):
                cols = pl.ds(pl.multiple_of(j * TW, TW), TW)
                store(cols, own[slot, r, cols] + rA[l, c, r, cols].astype(F32))
                return 0

            lax.fori_loop(0, G // TW, body, 0, unroll=True)
            blk = own[slot, r, G:] + rA[l, c, r, G:].astype(F32)
            last(split(blk[:, 0:1] + blk[:, LANES // 2:LANES // 2 + 1]))

        for d in range(1, NY):
            p = ypeer(d)

            def put(cols, v, d=d):
                sB[l, c, d - 1, :, cols] = v.astype(BF16)

            def put_last(v, d=d):
                sB[l, c, d - 1, :, G:] = v.astype(BF16)

            reduced(p, put, put_last)
            send(("b", l, c, d), sB.at[l, c, d - 1], rB.at[l, c, d - 1], bs_, br_.at[l, c, d - 1],
                 ra=p * CORES + core)

        def keep(cols, v):
            own2[slot, :, cols] = v

        def keep_last(v):
            own2[slot, :, G:] = v

        reduced(y, keep, keep_last)

    def stage_c(l, c):
        slot = c
        for d in range(1, NY):
            flight["b", l, c, d].wait_recv()

        def total(cols):
            t = own2[slot, :, cols]
            for d in range(1, NY):
                t += rB[l, c, d - 1, :, cols].astype(F32)
            return t

        blk = total(pl.ds(G, LANES))
        sq = blk[:, 0:1] + blk[:, LANES // 2:LANES // 2 + 1]
        factor = lax.rsqrt(sq / D + 1e-6)

        def body(j, _):
            at = pl.multiple_of(j * LANES, LANES)
            cols = pl.ds(at, LANES)
            gate = total(cols) * factor * gsc_v[l, cols].reshape(1, LANES)
            up = total(pl.ds(pl.multiple_of(Fp + at, LANES), LANES)) * factor * usc_v[l, cols].reshape(1, LANES)
            H[l, c, core, y, :, cols] = (gate / (1.0 + jnp.exp(-gate)) * up).astype(BF16)
            return 0

        lax.fori_loop(0, Fp // LANES, body, 0, unroll=True)
        mine = H.at[l, c, core, y]
        for d in range(1, NY):
            send(("c", l, c, d), mine, mine, cs_, cr_.at[l, c, d - 1], ra=ypeer(d) * CORES + core)
        send(("p", l, c, 0), mine, mine, ps_, pr_.at[l, c, 0], ra=partner)

    def stage_f(l, c):
        for d in range(1, NY):
            flight["c", l, c, d].wait_recv()
            theirs = H.at[l, c, core, lax.rem(y + NY - d, NY)]
            send(("p", l, c, d), theirs, theirs, ps_, pr_.at[l, c, d], ra=partner)

    def stage_d_(l, c):
        for d in range(NY):
            flight["p", l, c, d].wait_recv()

        def body(j, _):
            cols = pl.ds(pl.multiple_of(j * TD, TD), TD)
            h = H[l, c].reshape(T, Fp)
            PD[l, c, :, cols] = jnp.dot(h, wdn[l, :, cols], preferred_element_type=F32).astype(BF16)
            return 0

        lax.fori_loop(0, Dk // TD, body, 0, unroll=True)
        halves = []
        for k, rows in enumerate((other_rows, mine_rows)):
            halves.append(ready(PD.at[l, c, rows], rD.at[l, c, rows], ds_, dr_.at[l, c, k], cb=inner))
        flight["d", l, c] = halves

        @pl.when(jnp.logical_and(end, not_middle))
        def _():
            for copy in halves:
                copy.start()

    def stage_e1(l, c):
        halves = flight["d", l, c]
        across = ready(sX.at[l, c], rX.at[l, c], xs_, xr_.at[l, c], cb=inner)
        flight["x", l, c] = across

        if NZ > 4:
            @pl.when(jnp.logical_and(not_end, not_middle))
            def _():
                for copy, rows in zip(halves, (other_rows, mine_rows)):
                    copy.wait_recv()
                    PD[l, c, rows, :] = (PD[l, c, rows, :].astype(F32) + rD[l, c, rows, :].astype(F32)).astype(BF16)
                    copy.start()

        @pl.when(middle)
        def _():
            give = PD[l, c, other_rows, :].astype(F32)
            if NZ > 2:
                halves[0].wait_recv()
                give += rD[l, c, other_rows, :].astype(F32)
            sX[l, c] = give.astype(BF16)
            across.start()

    def stage_e2(l, c):
        halves, across = flight["d", l, c], flight["x", l, c]
        mine = M.at[l, c, mine_rows]
        outs = []
        for k in range(1, NZ):
            d = NZ - k
            outs.append(ready(mine, mine, es_.at[k - 1], er_.at[l, c, side], cb=zpeer(d)))

        @pl.when(middle)
        def _():
            t = PD[l, c, mine_rows, :].astype(F32)
            if NZ > 2:
                halves[1].wait_recv()
                t += rD[l, c, mine_rows, :].astype(F32)
            across.wait_recv()
            t += rX[l, c].astype(F32)
            a = acts_rows(l, c, side * half, half).astype(F32)
            M[l, c, mine_rows, :] = (0.5 * a + 0.5 * (t * dsc_v[l, :].reshape(1, Dk))).astype(BF16)
            for copy in outs:
                copy.start()

    def arrived(l, c):
        @pl.when(not_middle)
        def _():
            wait_half(l, c, mine_rows, side)

        wait_half(l, c, other_rows, 1 - side)

    def finish(c):
        arrived(1, c)
        out_ref[c * T:(c + 1) * T, :] = M[1, c]

    names = (stage_a, stage_b, stage_c, stage_f, stage_d_, stage_e1, stage_e2)
    todo = []
    for c in range(C):
        for l in range(2):
            for name, at in zip(names, OFFSETS):
                todo.append((l * LAYER + c * PERIOD + at, functools.partial(name, l, c)))
        todo.append((2 * LAYER + c * PERIOD, functools.partial(finish, c)))
    todo.append((OFFSETS[4] - 0.01, functools.partial(cast_down, 0)))
    todo.append((LAYER - 0.2, functools.partial(cast_up, 1)))
    todo.append((LAYER - 0.1, functools.partial(cast_down, 1)))

    cast_up(0)
    load_rest()
    for copy in inputs:
        copy.wait()
    pl.semaphore_wait(barrier, 1 + (NY - 1) + (NZ - 1))
    for _, stage in sorted(todo, key=lambda item: item[0]):
        stage()
    all_sent(sA, as_)
    all_sent(sB, bs_)
    all_sent(H.at[:, :, 0, pl.ds(0, NY - 1)], cs_)
    all_sent(H.at[:, :, 0], ps_)

    @pl.when(not_middle)
    def _():
        all_sent(PD, ds_)

    @pl.when(middle)
    def _():
        all_sent(sX, xs_)
        for k in range(NZ - 1):
            all_sent(sX, es_.at[k])


def local(NY, NZ, x, g1, wg1, gs1, wu1, us1, wd1, ds1, g2, wg2, gs2, wu2, us2, wd2, ds2):
    tokens, Dk = x.shape
    F = wg1.shape[1]
    Fp = -(-F // LANES) * LANES
    D = Dk * NY * CORES
    C = next(c for c in (8, 4, 2, 1) if tokens % (c * 16 * NY * CORES) == 0)
    T = tokens // C
    half, tr = T // CORES, T // CORES // NY
    W = 2 * Fp + LANES

    def padded(v):
        return jnp.pad(v, (0, Fp - F)) if F != Fp else v

    small = [x, g1, padded(gs1), padded(us1), ds1, g2, padded(gs2), padded(us2), ds2]
    weights = [wg1, wu1, wd1, wg2, wu2, wd2]
    dma = pltpu.SemaphoreType.DMA
    return pl.pallas_call(
        functools.partial(kernel, (C, NY, NZ, T, Dk, F, Fp, D)),
        out_shape=pltpu.VMEM((tokens, Dk), BF16),
        in_specs=[pl.BlockSpec(memory_space=pl.ANY)] * 15,
        out_specs=pl.BlockSpec(memory_space=pltpu.VMEM),
        scratch_shapes=[
            pltpu.VMEM((tokens, Dk), BF16),
            pltpu.VMEM((2, Dk), F32),
            pltpu.VMEM((2, Fp), F32),
            pltpu.VMEM((2, Fp), F32),
            pltpu.VMEM((2, Dk), F32),
            pltpu.VMEM((2, Dk, F), F32),
            pltpu.VMEM((2, Dk, F), F32),
            pltpu.VMEM((2, F, Dk), F32),
            pltpu.VMEM((2, Dk, 2 * Fp), BF16),
            pltpu.VMEM((2, Fp, Dk), BF16),
            pltpu.VMEM((T, Dk), BF16),
            pltpu.VMEM((C, half, W), F32),
            pltpu.VMEM((C, tr, W), F32),
            pltpu.VMEM((2, C, half, W), BF16),
            pltpu.VMEM((2, C, half, W), BF16),
            pltpu.VMEM((2, C, NY - 1, tr, W), BF16),
            pltpu.VMEM((2, C, NY - 1, tr, W), BF16),
            pltpu.VMEM((2, C, CORES, NY, tr, Fp), BF16),
            pltpu.VMEM((2, C, T, Dk), BF16),
            pltpu.VMEM((2, C, T, Dk), BF16),
            pltpu.VMEM((2, C, half, Dk), BF16),
            pltpu.VMEM((2, C, half, Dk), BF16),
            pltpu.VMEM((2, C, T, Dk), BF16),
            dma, dma((2, 4)), dma((2, 3, 4)),
            dma, dma((2, C)),
            dma, dma((2, C, NY - 1)),
            dma, dma((2, C, NY - 1)),
            dma, dma((2, C, NY)),
            dma, dma((2, C, 2)),
            dma, dma((2, C)),
            dma((NZ - 1,)), dma((2, C, 2)),
        ],
        compiler_params=pltpu.CompilerParams(
            collective_id=0, has_side_effects=True, vmem_limit_bytes=58 * 1024 * 1024
        ),
    )(*small, *weights)


def solution(mesh):
    NY = mesh.shape["ra"] // CORES
    NZ = mesh.shape["cb"]
    return jax.shard_map(
        functools.partial(local, NY, NZ),
        mesh=mesh,
        in_specs=(
            P("grp", "ra"),
            P("ra"),
            P("ra", "cb"),
            P("cb"),
            P("ra", "cb"),
            P("cb"),
            P("cb", "ra"),
            P("ra"),
            P("ra"),
            P("ra", "cb"),
            P("cb"),
            P("ra", "cb"),
            P("cb"),
            P("cb", "ra"),
            P("ra"),
        ),
        out_specs=P("grp", "ra"),
        check_vma=False,
    )
```
